32 devices in a mesh: sp: 4 (over y, x), tp: 8 (over z, core).
Axes of the slice: x: 2, y: 2, z: 4, core: 2. Of those that a mesh axis runs over, the one named last changes fastest.
Arguments:
- mix_in: bfloat16 [4096, 2048], P('sp', 'tp'), may hold values from -8 to 8
- gate_in: bfloat16 [4096, 2048], P('sp', 'tp'), may hold values from -6 to 6
- conv_w: float32 [4, 2048], P(None, 'tp'), may hold values from -3 to 3
- conv_b: float32 [2048], P('tp'), may hold values from -3 to 3
- decay_param: float32 [2, 2048], P(None, 'tp')
- recur_gate: float32 [2, 32, 64, 64], P(None, 'tp'), may hold values from -0.75 to 0.75
- recur_bias: float32 [2, 2048], P(None, 'tp'), may hold values from -4 to 4
- input_gate: float32 [2, 32, 64, 64], P(None, 'tp'), may hold values from -0.75 to 0.75
- input_bias: float32 [2, 2048], P(None, 'tp'), may hold values from -4 to 4
- residual: bfloat16 [4096, 2048], P(('sp', 'tp')), may hold values from -6 to 6
- out_proj: bfloat16 [2048, 2048], replicated, may hold values from -0.125 to 0.125
- norm_gain: float32 [3, 2048], replicated, may hold values from 0.1 to 1.9
- routes: int32 [4096, 2], P('sp'), may hold values from 0 to 15, all different within a row; in each aligned block of 128 rows (0 to 127, 128 to 255, ...) at most 32 rows name the same one
- route_wt: float32 [4096, 2], P('sp'), may hold values from 0.1 to 1
- exp_gate: bfloat16 [16, 2048, 1024], P('sp', None, 'tp'), may hold values from -0.125 to 0.125
- exp_up: bfloat16 [16, 2048, 1024], P('sp', None, 'tp'), may hold values from -0.125 to 0.125
- exp_down: bfloat16 [16, 1024, 2048], P('sp', 'tp'), may hold values from -0.1875 to 0.1875
Outputs:
- final: bfloat16 [4096, 2048], P(('sp', 'tp'))
The draws below stay inside these ranges and needn't reach their ends.
Inputs may be any that keep to these rules, and one draw needn't show every extreme that they name: `routes`: in each aligned block of 128 tokens (the rows of one device in the expert layer) no expert is named more than 32 times, and in some block some expert exactly 32 times; a token's 2 experts differ.
All inputs are finite; a program needn't handle non-finite values.
Results may differ from the reference program's by a relative error of at most 0.008.
Values may be sent and summed in bfloat16 or wider, within the bound.
A program may use at most 128 MiB of HBM per device.

```python
import math
import jax
import jax.numpy as jnp
import numpy as np
from jax import lax

D = 2048
WIDTH = 2048
HEAD = 64
FF = 1024
EXPERTS = 16
TOPK = 2
SEQ_DEV = 1024
HEADS = 32
SEQ = 4096
ROWS = 128
CAP = 32


def draw_decay_param(key, part):
    pick_key, slow_key, fast_key = jax.random.split(jax.random.fold_in(key, 17), 3)
    slow_share = 0.5
    chooser = jax.random.uniform(pick_key, (2, WIDTH), jnp.float32)
    slow_values = math.log(SEQ) + jax.random.uniform(slow_key, (2, WIDTH), jnp.float32, 0.7, 1.7)
    fast_values = jax.random.uniform(fast_key, (2, WIDTH), jnp.float32, 3.5, 5.0)
    return jnp.where(chooser < slow_share, slow_values, fast_values).astype(jnp.float32)


def draw_conv_w(key, part):
    tap_key = jax.random.fold_in(key, 31)
    values = jax.random.normal(tap_key, (4, WIDTH), jnp.float32)
    tap_scale = jnp.array([0.4, 0.4, 0.4, 1.2], jnp.float32)[:, None]
    return jnp.clip(values * tap_scale, -3.0, 3.0).astype(jnp.float32)


def draw_mix_in(key, part):
    value_key, scale_key, offset_key = jax.random.split(jax.random.fold_in(key, 23), 3)
    values = jax.random.normal(value_key, (SEQ, WIDTH), jnp.float32)
    spread = 0.8
    position = jnp.arange(SEQ, dtype=jnp.int32) % SEQ_DEV
    at_ends = jnp.logical_or(position < 2, position >= SEQ_DEV - 2)
    values = values * jnp.where(at_ends, 3.0, 1.0)[:, None]
    scales = jnp.exp(jax.random.uniform(scale_key, (SEQ // 64, 1, WIDTH), jnp.float32, -spread, spread))
    shaped = (values.reshape(SEQ // 64, 64, WIDTH) * scales).reshape(SEQ, WIDTH)
    offsets = jax.random.uniform(offset_key, (SEQ // SEQ_DEV, 1, WIDTH), jnp.float32, -1.5, 1.5)
    shifted = (shaped.reshape(SEQ // SEQ_DEV, SEQ_DEV, WIDTH) + offsets).reshape(SEQ, WIDTH)
    return jnp.clip(shifted, -8.0, 8.0).astype(jnp.bfloat16)


def level_of(key, extent, shards, smallest, high):
    loudness, own = 1.0, jax.random.fold_in(key, 6)
    for dim, parts in shards:
        draws = jnp.exp(jax.random.uniform(jax.random.fold_in(own, dim), (parts,), jnp.float32, smallest / len(shards), high / len(shards)))
        loudness = loudness * jnp.repeat(draws, extent[dim] // parts).reshape([-1 if axis == dim else 1 for axis in range(len(extent))])
    return loudness


def deal_out(stream_key, own, number, rows, count, top, reach, lean):
    sequence = jax.random.permutation(stream_key, count)
    crowded, ordinary = load_shares(count, rows * top, reach, lean, True), load_shares(count, rows * top, reach, lean, False)
    places = jnp.arange(count)

    def named(tallies, rotation):
        used = int((tallies > 0).sum())
        fixed = max(1, used // 4)
        passed = fixed + (places - fixed + rotation * (used - fixed)) % max(1, count - fixed)
        return jnp.zeros((count,), jnp.int32).at[sequence[jnp.where(places < fixed, places, passed)]].set(jnp.asarray(tallies, jnp.int32))

    tallies = jnp.where(number % 4 == 0, named(crowded, number // 4), named(ordinary, number - number // 4 - 1))
    mixed = jax.random.permutation(jax.random.fold_in(own, 3), count)
    source_of, sink = mixed[0:count // 2 * 2:2], mixed[1:count // 2 * 2:2]
    room = jnp.minimum(tallies[source_of] - 1, reach - tallies[sink]) // 2
    room = jnp.where((source_of == sequence[0]) | (sink == sequence[0]) | (tallies[sink] == 0), 0, jnp.maximum(room, 0))
    passed = jax.random.randint(jax.random.fold_in(own, 4), (count // 2,), 0, 1 << 20) % (room + 1)
    tallies = tallies.at[source_of].add(-passed).at[sink].add(passed)
    items = jnp.searchsorted(jnp.cumsum(tallies), jnp.arange(rows * top), side="right").astype(jnp.int32)
    table = items.reshape(top, rows).T
    table = table[jax.random.permutation(jax.random.fold_in(own, 1), rows)]
    rotation = jax.random.randint(jax.random.fold_in(own, 2), (rows, 1), 0, top)
    return jnp.take_along_axis(table, (jnp.arange(top)[None, :] + rotation) % top, axis=1)


def load_shares(count, total, most, lean, full):
    portions = [(1 << 20) // math.isqrt(standing ** lean) + 1 for standing in range(1, count + 1)]
    largest = most if full else min(most, max(-(-total // count), total * portions[0] // sum(portions)))
    least = 1 if total - largest >= count - 1 else 0
    holding, surplus = [largest] + [least] * (count - 1), total - largest - least * (count - 1)
    while surplus > 0:
        movable = [i for i in range(1, count) if holding[i] < largest] or [i for i in range(1, count) if holding[i] < most]
        pool, budget = sum([portions[i] for i in movable]), surplus
        for i in movable:
            more = min(most - holding[i], max(1, budget * portions[i] // pool), surplus)
            holding[i] = holding[i] + more
            surplus = surplus - more
    return np.array(holding)


def centred(stream_key, dims, deviation, limit, cuts=(), held_as=jnp.bfloat16):
    entries = jax.random.normal(stream_key, dims, jnp.float32) * deviation
    if len(cuts) > 0:
        entries = level_of(stream_key, dims, cuts, -0.22, 0.18) * entries
    return jnp.clip(entries, min=-limit, max=limit).astype(held_as)


def setup_inputs(seed: int = 0) -> dict:
    splits = jax.random.split(jax.random.key(seed), 18)
    mix_in = draw_mix_in(jax.random.fold_in(splits[17], 71), 0)
    gate_in = centred(splits[1], (SEQ, WIDTH), 1.0, 6.0, ((0, 4), (1, 8)))
    conv_w = draw_conv_w(jax.random.fold_in(splits[17], 71), 0)
    conv_b = centred(splits[3], (WIDTH,), 0.5, 3.0, ((0, 8),), jnp.float32)
    decay_param = draw_decay_param(jax.random.fold_in(splits[17], 71), 0)
    recur_gate = centred(splits[5], (2, HEADS, HEAD, HEAD), HEAD ** -0.5, 0.75, ((1, 8),), jnp.float32)
    recur_bias = centred(splits[6], (2, WIDTH), 1.0, 4.0, ((1, 8),), jnp.float32)
    input_gate = centred(splits[7], (2, HEADS, HEAD, HEAD), HEAD ** -0.5, 0.75, ((1, 8),), jnp.float32)
    input_bias = centred(splits[8], (2, WIDTH), 1.0, 4.0, ((1, 8),), jnp.float32)
    residual = centred(splits[9], (SEQ, D), 1.0, 6.0, ((0, 32),))
    out_proj = centred(splits[10], (WIDTH, D), WIDTH ** -0.5, 0.125)
    norm_gain = jnp.clip(1.0 + 0.18 * jax.random.normal(splits[11], (3, D), jnp.float32), 0.1, 1.9)
    routes_keys = jax.random.split(jax.random.fold_in(splits[12], 1), SEQ // ROWS)
    routes_turns = jax.random.permutation(jax.random.fold_in(splits[12], 3), SEQ // ROWS)
    routes = jax.vmap(lambda own, number: deal_out(jax.random.fold_in(splits[12], 2), own, number, ROWS, EXPERTS, TOPK, CAP, 2))(routes_keys, routes_turns).reshape((SEQ, TOPK))
    route_wt = jnp.clip(0.1 + 0.9 * jax.random.uniform(splits[13], (SEQ, TOPK), jnp.float32) ** level_of(splits[13], (SEQ, TOPK), ((0, 4),), -0.2, 0.2), 0.1, 1.0)
    exp_gate = centred(splits[14], (EXPERTS, D, FF), D ** -0.5, 0.125, ((0, 4), (2, 8)))
    exp_up = centred(splits[15], (EXPERTS, D, FF), D ** -0.5, 0.125, ((0, 4), (2, 8)))
    exp_down = centred(splits[16], (EXPERTS, FF, D), FF ** -0.5, 0.1875, ((0, 4), (1, 8)))
    return {"mix_in": mix_in, "gate_in": gate_in, "conv_w": conv_w, "conv_b": conv_b, "decay_param": decay_param, "recur_gate": recur_gate, "recur_bias": recur_bias, "input_gate": input_gate, "input_bias": input_bias, "residual": residual, "out_proj": out_proj, "norm_gain": norm_gain, "routes": routes, "route_wt": route_wt, "exp_gate": exp_gate, "exp_up": exp_up, "exp_down": exp_down}


EPSILON = 1e-06
HIGHEST_MODE = lax.Precision.HIGHEST

def norm_rows(values, gain):
    floats = values.astype(jnp.float32)
    return floats * lax.rsqrt(lax.optimization_barrier(jnp.mean(floats * floats, axis=-1, keepdims=True)) + EPSILON) * gain

def pair_join(earlier, later_pair):
    return (earlier[0] * later_pair[0], later_pair[0] * earlier[1] + later_pair[1])

def slot_table(route_rows, experts, capacity):
    row_count, top_count = route_rows.shape
    flattened = route_rows.reshape(row_count * top_count)
    matches = (flattened[:, None] == jnp.arange(experts, dtype=jnp.int32)[None, :]).astype(jnp.int32)
    earlier_hits = jnp.cumsum(matches, axis=0) - matches
    position = lax.optimization_barrier(jnp.sum(earlier_hits * matches, axis=1))
    return (flattened * capacity + position).reshape(row_count, top_count)

def coefficients(conv_out, recur_blocks, recur_bias, input_blocks, input_bias, decay_param):
    seq_len, channels = conv_out.shape
    heads, head_dim, _ = recur_blocks.shape
    blocked = conv_out.reshape(seq_len, heads, head_dim)
    recur_pre = jnp.einsum('lhi,hij->lhj', blocked, recur_blocks, precision=HIGHEST_MODE).reshape(seq_len, channels)
    input_pre = jnp.einsum('lhi,hij->lhj', blocked, input_blocks, precision=HIGHEST_MODE).reshape(seq_len, channels)
    recur_act = jax.nn.sigmoid(recur_pre + recur_bias)
    input_act = jax.nn.sigmoid(input_pre + input_bias)
    log_decay = -8.0 * recur_act * jax.nn.softplus(-decay_param)
    return (jnp.exp(log_decay), jnp.sqrt(-jnp.expm1(2.0 * log_decay)) * (input_act * conv_out))

def expert_apply(operands):
    tokens_in, gate_w, up_w, down_w = operands
    gate_act = jnp.dot(tokens_in, gate_w, preferred_element_type=jnp.float32)
    up_act = jnp.dot(tokens_in, up_w, preferred_element_type=jnp.float32)
    hidden = (jax.nn.silu(gate_act) * up_act).astype(jnp.bfloat16)
    return jnp.dot(hidden, down_w, preferred_element_type=jnp.float32).astype(jnp.bfloat16)

def reference(mix_in, gate_in, conv_w, conv_b, decay_param, recur_gate, recur_bias, input_gate, input_bias, residual, out_proj, norm_gain, routes, route_wt, exp_gate, exp_up, exp_down):
    seq_len = mix_in.shape[0]
    padded = jnp.pad(mix_in.astype(jnp.float32), ((2, 1), (0, 0)))
    conv_out = conv_b + padded[0:seq_len] * conv_w[0]
    for tap in range(1, conv_w.shape[0]):
        conv_out = conv_out + padded[tap:tap + seq_len] * conv_w[tap]
    state_sum = jnp.zeros_like(conv_out)
    for sense in range(2):
        decay, drive = coefficients(conv_out, recur_gate[sense], recur_bias[sense], input_gate[sense], input_bias[sense], decay_param[sense])
        if sense == 1:
            decay, drive = (jnp.flip(decay, 0), jnp.flip(drive, 0))
        _, states = lax.associative_scan(pair_join, (decay, drive), axis=0)
        if sense == 1:
            states = jnp.flip(states, 0)
        state_sum = state_sum + states
    mixed = (state_sum * jax.nn.gelu(gate_in.astype(jnp.float32))).astype(jnp.bfloat16)
    proj = jnp.dot(mixed, out_proj, preferred_element_type=jnp.float32).astype(jnp.bfloat16)
    proj = lax.optimization_barrier(proj)
    stream = (residual.astype(jnp.float32) + norm_rows(proj, norm_gain[0])).astype(jnp.bfloat16)
    stream = lax.optimization_barrier(stream)
    normed = norm_rows(stream, norm_gain[1]).astype(jnp.bfloat16)
    nblocks = seq_len // ROWS
    route_blocks = routes.reshape(nblocks, ROWS, TOPK)
    slots = jax.vmap(lambda block: slot_table(block, EXPERTS, CAP))(route_blocks)
    source_rows = jnp.repeat(jnp.arange(ROWS, dtype=jnp.int32), TOPK)

    def fill_table(slot_rows):
        empty = jnp.full((EXPERTS * CAP,), ROWS, jnp.int32)
        return empty.at[slot_rows.reshape(ROWS * TOPK)].set(source_rows)
    table = jax.vmap(fill_table)(slots)
    blocks_pad = jnp.concatenate([normed.reshape(nblocks, ROWS, D), jnp.zeros((nblocks, 1, D), jnp.bfloat16)], axis=1)
    dispatched = jnp.take_along_axis(blocks_pad, table[:, :, None], axis=1)
    by_expert = jnp.moveaxis(dispatched.reshape(nblocks, EXPERTS, CAP, D), 1, 0).reshape(EXPERTS, nblocks * CAP, D)
    results = lax.map(expert_apply, (by_expert, exp_gate, exp_up, exp_down)).reshape(EXPERTS, nblocks, CAP, D)
    slot_place = (slots % CAP).astype(jnp.int32)
    expert_ids = (slots // CAP).astype(jnp.int32)
    block_ids = jnp.arange(nblocks, dtype=jnp.int32)[:, None, None]
    picked = results[expert_ids, block_ids, slot_place]
    weights = route_wt.reshape(nblocks, ROWS, TOPK)[..., None]
    mixture = lax.optimization_barrier(jnp.sum(weights * picked.astype(jnp.float32), axis=2)).reshape(seq_len, D).astype(jnp.bfloat16)
    mixture = lax.optimization_barrier(mixture)
    return (stream.astype(jnp.float32) + norm_rows(mixture, norm_gain[2])).astype(jnp.bfloat16)
```

```python
import functools

import jax
import jax.numpy as jnp
from jax import lax
from jax.experimental import pallas as pl
from jax.experimental.pallas import tpu as pltpu
from jax.sharding import PartitionSpec as P

EPSILON = 1e-06
HIGHEST_MODE = lax.Precision.HIGHEST
MESH = pl.DeviceIdType.MESH
HALO = 16
SUB = 8


def norm_rows(values, gain):
    floats = values.astype(jnp.float32)
    return floats * lax.rsqrt(jnp.mean(floats * floats, axis=-1, keepdims=True) + EPSILON) * gain


def slot_table(route_rows, experts, capacity):
    row_count, top_count = route_rows.shape
    flattened = route_rows.reshape(row_count * top_count)
    matches = flattened[:, None] == jnp.arange(experts, dtype=jnp.int32)[None, :]
    order = jnp.arange(row_count * top_count, dtype=jnp.int32)
    before = (order[None, :] < order[:, None]).astype(jnp.bfloat16)
    earlier_hits = jnp.dot(
        before, matches.astype(jnp.bfloat16), preferred_element_type=jnp.float32
    )
    position = jnp.sum(jnp.where(matches, earlier_hits, 0.0), axis=1).astype(jnp.int32)
    return (flattened * capacity + position).reshape(row_count, top_count)


def weight_table(slots, route_weights, total_slots):
    matches = slots[..., None] == jnp.arange(total_slots, dtype=jnp.int32)
    return jnp.sum(jnp.where(matches, route_weights[..., None], 0.0), axis=-2)


def one_minus_exp(y):
    series = -y * (1.0 + y * (1.0 / 2) * (1.0 + y * (1.0 / 3) * (1.0 + y * 0.25 * (1.0 + y * 0.2))))
    return jnp.where(y > -0.1, series, 1.0 - jnp.exp(y))


def split_f32(x):
    high = x.astype(jnp.bfloat16)
    return high, (x - high.astype(jnp.float32)).astype(jnp.bfloat16)


def tile_scan(a, b, reverse):
    row = lax.broadcasted_iota(jnp.int32, a.shape, 1)
    step = 1
    while step < SUB:
        shift = SUB - step if reverse else step
        keep = row < SUB - step if reverse else row >= step
        a_prev = jnp.where(keep, pltpu.roll(a, shift, 1), 1.0)
        b_prev = jnp.where(keep, pltpu.roll(b, shift, 1), 0.0)
        b = b + a * b_prev
        a = a * a_prev
        step *= 2
    return a, b


def mixer_kernel(
    dims,
    mix_ref, gate_ref, cw_ref, cb_ref, soft_ref, rg_ref, rb_ref, ig_ref, ib_ref,
    res_ref, gain_ref, slots_ref, op_hbm, eg_hbm, eu_hbm, ed_hbm,
    stream_ref, arrived_hbm, gf_hbm, uf_hbm, df_hbm,
    xp, wh, wl, af, bf, ab, bb, mixed, tok, op, proj, outgoing, halo, summ, ends,
    bg, bu, bd,
    op_sem, own_sem, halo_send, halo_recv, sum_send, sum_recv,
    mix_send, mix_recv, dis_send, dis_recv, z_send, z_recv, c_send, c_recv,
):
    S, T, L, G = dims
    seq, C = mix_ref.shape
    rows, D = res_ref.shape
    slots = outgoing.shape[0]
    cap = slots // (S * L)
    heads, hd = rg_ref.shape[1], rg_ref.shape[2]
    F = eg_hbm.shape[2]
    sp = lax.axis_index("sp")
    tp = lax.axis_index("tp")
    q = tp // G
    g = lax.rem(tp, G)

    def place_of(dq, dg):
        return lax.rem(q + dq, L) * G + lax.rem(g + dg, G)

    op_copy = pltpu.make_async_copy(op_hbm, op, op_sem)
    op_copy.start()
    own_in = [
        pltpu.make_async_copy(h.at[q], v, own_sem.at[i])
        for i, (h, v) in enumerate(((eg_hbm, bg), (eu_hbm, bu), (ed_hbm, bd)))
    ]
    for c in own_in:
        c.start()

    barrier = pltpu.get_barrier_semaphore()
    greeted = 0
    for ds in range(S):
        for dq in range(L):
            for dg in range(G):
                if (ds or dq or dg) and (ds == 0 or dg == 0):
                    pl.semaphore_signal(
                        barrier, inc=1,
                        device_id=(lax.rem(sp + ds, S), place_of(dq, dg)),
                        device_id_type=MESH,
                    )
                    greeted += 1
    pl.semaphore_wait(barrier, greeted)

    def remote(src, dst, send, recv, sp_to, tp_to):
        return pltpu.make_async_remote_copy(
            src_ref=src, dst_ref=dst, send_sem=send, recv_sem=recv,
            device_id=(sp_to, tp_to), device_id_type=MESH,
        )

    to_next = remote(mix_ref.at[pl.ds(seq - HALO, HALO)], halo.at[0], halo_send.at[0],
                     halo_recv.at[0], lax.rem(sp + 1, S), tp)
    to_prev = remote(mix_ref.at[pl.ds(0, HALO)], halo.at[1], halo_send.at[1],
                     halo_recv.at[1], lax.rem(sp + S - 1, S), tp)
    to_next.start()
    to_prev.start()

    def full_slot(ref, axis, place):
        if len(ref.shape) == 3:
            return ref.at[place]
        start = pl.multiple_of(place * F, F)
        return ref.at[:, pl.ds(start, F)] if axis else ref.at[pl.ds(start, F), :]

    tensors = ((eg_hbm, gf_hbm, 1), (eu_hbm, uf_hbm, 1), (ed_hbm, df_hbm, 0))

    def z_copies(dq):
        return [
            remote(src.at[lax.rem(q + dq, L)], full_slot(dst, axis, tp), z_send.at[dq, i],
                   z_recv.at[dq, i], sp, place_of(dq, 0))
            for i, (src, dst, axis) in enumerate(tensors)
        ]

    def core_copies(dq, i, own):
        src, dst, axis = tensors[i]
        origin = place_of(L - dq, 0)
        at = full_slot(dst, axis, origin)
        return [
            remote(own if own is not None else at, at, c_send.at[dq, dg, i], c_recv.at[dq, dg, i],
                   sp, place_of(0, dg))
            for dg in range(1, G)
        ]

    far = [dq for dq in range(1, L) if min(dq, L - dq) > 1]
    near = [dq for dq in range(1, L) if min(dq, L - dq) == 1]
    z_all = {dq: z_copies(dq) for dq in range(1, L)}
    for i in range(3):
        for dq in near:
            z_all[dq][i].start()
    own_out, core_all = [], {}
    for i, (src, dst, axis) in enumerate(tensors):
        core_all[0, i] = core_copies(0, i, src.at[q])
        for c in core_all[0, i]:
            c.start()
    for i, (buf, (src, dst, axis)) in enumerate(zip((bg, bu, bd), tensors)):
        own_in[i].wait()
        c = pltpu.make_async_copy(buf, full_slot(dst, axis, tp), own_sem.at[3 + i])
        c.start()
        own_out.append(c)

    wh[...] = jnp.zeros_like(wh)
    wl[...] = jnp.zeros_like(wl)
    for k, ref in enumerate((rg_ref, ig_ref)):
        for sense in range(2):
            for h in range(heads):
                high, low = split_f32(ref[sense, h])
                col = (2 * sense + k) * C + h * hd
                wh[h * hd : (h + 1) * hd, col : col + hd] = high
                wl[h * hd : (h + 1) * hd, col : col + hd] = low
    xp[SUB : SUB + seq, :] = mix_ref[...].astype(jnp.float32)
    to_next.wait()
    to_prev.wait()
    tail = halo[0].astype(jnp.float32)[HALO - SUB : HALO]
    head = halo[1].astype(jnp.float32)[0:SUB]
    xp[0:SUB, :] = jnp.where(sp > 0, tail, 0.0)
    xp[SUB + seq : 2 * SUB + seq, :] = jnp.where(sp < S - 1, head, 0.0)

    R = min(128, seq)

    def gates(n, _):
        base = pl.multiple_of(n * R, R)
        window = xp[pl.ds(base, R + 2 * SUB), :]
        conv = cb_ref[...] + window[SUB - 2 : SUB - 2 + R] * cw_ref[0:1]
        for tap in range(1, cw_ref.shape[0]):
            conv = conv + window[SUB - 2 + tap : SUB - 2 + tap + R] * cw_ref[tap : tap + 1]
        high, low = split_f32(conv)
        for sense, (a_ref, b_ref) in enumerate(((af, bf), (ab, bb))):
            cols = slice(2 * sense * C, (2 * sense + 2) * C)
            pre = jnp.dot(high, wh[:, cols], preferred_element_type=jnp.float32)
            pre = pre + jnp.dot(low, wh[:, cols], preferred_element_type=jnp.float32)
            pre = pre + jnp.dot(high, wl[:, cols], preferred_element_type=jnp.float32)
            recur = jax.nn.sigmoid(pre[:, :C] + rb_ref[sense : sense + 1])
            inp = jax.nn.sigmoid(pre[:, C:] + ib_ref[sense : sense + 1])
            log_a = -8.0 * recur * soft_ref[sense : sense + 1]
            a = jnp.exp(log_a)
            b = jnp.sqrt(one_minus_exp(2.0 * log_a)) * (inp * conv)
            a, b = tile_scan(
                a.reshape(R // SUB, SUB, C), b.reshape(R // SUB, SUB, C), sense == 1
            )
            a_ref[pl.ds(base, R), :] = a.reshape(R, C)
            b_ref[pl.ds(base, R), :] = b.reshape(R, C)
        return 0

    lax.fori_loop(0, seq // R, gates, 0)

    tiles = seq // SUB

    def carry(t, held):
        sf, pf, sb, pb = held
        at = pl.ds(pl.multiple_of(t * SUB, SUB), SUB)
        a = af[at, :]
        s = bf[at, :] + a * sf
        p = a * pf
        af[at, :] = p
        bf[at, :] = s
        back = pl.ds(pl.multiple_of((tiles - 1 - t) * SUB, SUB), SUB)
        a = ab[back, :]
        s2 = bb[back, :] + a * sb
        p2 = a * pb
        ab[back, :] = p2
        bb[back, :] = s2
        return s[SUB - 1 : SUB], p[SUB - 1 : SUB], s2[0:1], p2[0:1]

    zero, one = jnp.zeros((1, C), jnp.float32), jnp.ones((1, C), jnp.float32)
    sf, pf, sb, pb = lax.fori_loop(0, tiles, carry, (zero, one, zero, one), unroll=4)
    summ[0:1, :] = sf
    summ[1:2, :] = pf
    summ[2:3, :] = sb
    summ[3:4, :] = pb
    sums = [
        remote(summ, ends.at[ds - 1], sum_send.at[ds - 1], sum_recv.at[ds - 1],
               lax.rem(sp + ds, S), tp)
        for ds in range(1, S)
    ]
    for c in sums:
        c.start()
    for c in sums:
        c.wait()
    fe, be = zero, zero
    for ds in range(S - 1, 0, -1):
        fe = jnp.where(sp >= ds, ends[ds - 1, 1:2, :] * fe + ends[ds - 1, 0:1, :], fe)
    for ds in range(1, S):
        be = jnp.where(sp + S - ds < S, ends[ds - 1, 3:4, :] * be + ends[ds - 1, 2:3, :], be)

    def join(n, _):
        at = pl.ds(pl.multiple_of(n * R, R), R)
        state = (bf[at, :] + af[at, :] * fe) + (bb[at, :] + ab[at, :] * be)
        mixed[at, :] = (state * jax.nn.gelu(gate_ref[at, :].astype(jnp.float32))).astype(
            jnp.bfloat16
        )
        return 0

    lax.fori_loop(0, seq // R, join, 0)

    def block_rows(place):
        return mixed.at[pl.ds(pl.multiple_of(place * rows, rows), rows), :]

    columns = pl.ds(pl.multiple_of(tp * C, C), C)
    moves = []
    for dq in range(L):
        for dg in range(G):
            if dq or dg:
                k = dq * G + dg
                to = place_of(dq, dg)
                moves.append(remote(block_rows(to), tok.at[:, columns], mix_send.at[k],
                                    mix_recv.at[k], sp, to))
    for c in moves:
        c.start()
    own_move = pltpu.make_async_copy(block_rows(tp), tok.at[:, columns], own_sem.at[6])
    own_move.start()
    for dq in far:
        for c in z_all[dq]:
            c.start()
    op_copy.wait()
    own_move.wait()
    for c in moves:
        c.wait()

    def project(n, _):
        cols = pl.ds(pl.multiple_of(n * 256, 256), 256)
        proj[:, cols] = (
            jnp.dot(tok[...], op[:, cols], preferred_element_type=jnp.float32)
            .astype(jnp.bfloat16)
        )
        return 0

    lax.fori_loop(0, D // 256, project, 0)
    part = 32

    def norms(n, _):
        at = pl.ds(pl.multiple_of(n * part, part), part)
        s = (
            res_ref[at, :].astype(jnp.float32) + norm_rows(proj[at, :], gain_ref[0:1, :])
        ).astype(jnp.bfloat16)
        stream_ref[at, :] = s
        tok[at, :] = norm_rows(s, gain_ref[1:2, :]).astype(jnp.bfloat16)
        return 0

    lax.fori_loop(0, rows // part, norms, 0)
    slot_id = lax.broadcasted_iota(jnp.int32, (slots, rows), 0)
    hit = slot_id == slots_ref[0:1, :]
    for k in range(1, slots_ref.shape[0]):
        hit = hit | (slot_id == slots_ref[k : k + 1, :])
    selector = jnp.where(hit, 1.0, 0.0).astype(jnp.bfloat16)

    def dispatch(n, _):
        cols = pl.ds(pl.multiple_of(n * 256, 256), 256)
        outgoing[:, cols] = (
            jnp.dot(selector, tok[:, cols], preferred_element_type=jnp.float32)
            .astype(jnp.bfloat16)
        )
        return 0

    lax.fori_loop(0, D // 256, dispatch, 0)
    sends = []
    mine = sp * L + q
    for ds in range(S):
        for dq in range(L):
            sp_to, q_to = lax.rem(sp + ds, S), lax.rem(q + dq, L)
            src = outgoing.at[pl.ds(pl.multiple_of((sp_to * L + q_to) * cap, cap), cap), :]
            if ds or dq:
                k = ds * L + dq
                sends.append(remote(src, arrived_hbm.at[mine], dis_send.at[k], dis_recv.at[k],
                                    sp_to, q_to * G + g))
            else:
                sends.append(pltpu.make_async_copy(src, arrived_hbm.at[mine], own_sem.at[7]))
    for c in sends:
        c.start()
    for dq in near + far:
        for i in range(3):
            z_all[dq][i].wait_recv()
            core_all[dq, i] = core_copies(dq, i, None)
            for c in core_all[dq, i]:
                c.start()
    for c in sends:
        c.wait()
    for dq in range(1, L):
        for c in z_all[dq]:
            c.wait_send()
    for c in own_out:
        c.wait()
    for group in core_all.values():
        for c in group:
            c.wait()


def return_kernel(dims, rows_hbm, back_hbm, own_sem, send, recv):
    S, T, L, G = dims
    sp = lax.axis_index("sp")
    tp = lax.axis_index("tp")
    q = tp // G
    g = lax.rem(tp, G)
    barrier = pltpu.get_barrier_semaphore()
    peers = [
        (ds, dq, lax.rem(sp + ds, S), lax.rem(q + dq, L))
        for ds in range(S) for dq in range(L) if ds or dq
    ]
    for ds, dq, sp_to, q_to in peers:
        pl.semaphore_signal(
            barrier, inc=1, device_id=(sp_to, q_to * G + g), device_id_type=MESH
        )
    pl.semaphore_wait(barrier, len(peers))
    mine = sp * L + q
    copies = [
        pltpu.make_async_remote_copy(
            src_ref=rows_hbm.at[sp_to * L + q_to], dst_ref=back_hbm.at[mine],
            send_sem=send.at[ds * L + dq], recv_sem=recv.at[ds * L + dq],
            device_id=(sp_to, q_to * G + g), device_id_type=MESH,
        )
        for ds, dq, sp_to, q_to in peers
    ]
    copies.append(pltpu.make_async_copy(rows_hbm.at[mine], back_hbm.at[mine], own_sem))
    for c in copies:
        c.start()
    for c in copies:
        c.wait()


def on_device(
    mix_in, gate_in, conv_w, conv_b, decay_param, recur_gate, recur_bias, input_gate, input_bias,
    residual, out_proj, norm_gain, routes, route_wt, exp_gate, exp_up, exp_down,
):
    S, T = lax.axis_size("sp"), lax.axis_size("tp")
    L, D, F = exp_gate.shape
    G = T // L
    dims = (S, T, L, G)
    seq, C = mix_in.shape
    rows = residual.shape[0]
    top_count = routes.shape[1]
    experts = L * S
    cap = 2 * rows * top_count // experts
    total_slots = experts * cap
    own_start = lax.axis_index("tp") * rows
    own_routes = lax.dynamic_slice_in_dim(routes, own_start, rows, 0)
    own_weights = lax.dynamic_slice_in_dim(route_wt, own_start, rows, 0)
    own_slots = slot_table(own_routes, experts, cap)
    soft = jax.nn.softplus(-decay_param)
    wide = F % 128 == 0
    vmem = pl.BlockSpec(memory_space=pltpu.VMEM)
    hbm = pl.BlockSpec(memory_space=pltpu.MemorySpace.HBM)
    b16, f32 = jnp.bfloat16, jnp.float32
    dma = pltpu.SemaphoreType.DMA
    sds = jax.ShapeDtypeStruct
    up_shape = (D, T * F) if wide else (T, D, F)
    down_shape = (T * F, D) if wide else (T, F, D)
    stream, arrived, gate_full, up_full, down_full = pl.pallas_call(
        functools.partial(mixer_kernel, dims),
        out_shape=(
            sds((rows, D), b16), sds((experts, cap, D), b16),
            sds(up_shape, b16), sds(up_shape, b16), sds(down_shape, b16),
        ),
        in_specs=[vmem] * 12 + [hbm] * 4,
        out_specs=(vmem, hbm, hbm, hbm, hbm),
        scratch_shapes=[
            pltpu.VMEM((seq + 2 * SUB, C), f32),
            pltpu.VMEM((C, 4 * C), b16),
            pltpu.VMEM((C, 4 * C), b16),
            pltpu.VMEM((seq, C), f32), pltpu.VMEM((seq, C), f32),
            pltpu.VMEM((seq, C), f32), pltpu.VMEM((seq, C), f32),
            pltpu.VMEM((seq, C), b16),
            pltpu.VMEM((rows, T * C), b16),
            pltpu.VMEM(out_proj.shape, b16),
            pltpu.VMEM((rows, D), b16),
            pltpu.VMEM((total_slots, D), b16),
            pltpu.VMEM((2, HALO, C), b16),
            pltpu.VMEM((SUB, C), f32),
            pltpu.VMEM((S - 1, SUB, C), f32),
            pltpu.VMEM((D, F), b16), pltpu.VMEM((D, F), b16), pltpu.VMEM((F, D), b16),
            dma, dma((8,)),
            dma((2,)), dma((2,)),
            dma((S - 1,)), dma((S - 1,)),
            dma((T,)), dma((T,)),
            dma((experts,)), dma((experts,)),
            dma((L, 3)), dma((L, 3)),
            dma((L, G, 3)), dma((L, G, 3)),
        ],
        compiler_params=pltpu.CompilerParams(
            collective_id=0, has_side_effects=True, vmem_limit_bytes=56 * 1024 * 1024
        ),
    )(
        mix_in, gate_in, conv_w, conv_b.reshape(1, C), soft, recur_gate, recur_bias, input_gate,
        input_bias, residual, norm_gain, own_slots.T, out_proj, exp_gate, exp_up, exp_down,
    )
    flat = arrived.reshape(total_slots, D)
    if wide:
        gate_act = jnp.dot(flat, gate_full, preferred_element_type=f32)
        up_act = jnp.dot(flat, up_full, preferred_element_type=f32)
    else:
        gate_act = jnp.einsum("md,tdf->mtf", flat, gate_full, preferred_element_type=f32)
        up_act = jnp.einsum("md,tdf->mtf", flat, up_full, preferred_element_type=f32)
    hidden = (jax.nn.silu(gate_act) * up_act).astype(b16).reshape(total_slots, T * F)
    out_rows = jnp.dot(
        hidden, down_full.reshape(T * F, D), preferred_element_type=f32
    ).astype(b16)
    returned = pl.pallas_call(
        functools.partial(return_kernel, dims),
        out_shape=sds((experts, cap, D), b16),
        in_specs=[hbm],
        out_specs=hbm,
        scratch_shapes=[dma, dma((experts,)), dma((experts,))],
        compiler_params=pltpu.CompilerParams(collective_id=1, has_side_effects=True),
    )(out_rows.reshape(experts, cap, D))
    values = returned.reshape(total_slots, D).astype(f32)
    own_table = weight_table(own_slots, own_weights, total_slots)
    mixture = jnp.dot(own_table, values, precision=HIGHEST_MODE).astype(b16)
    mixture = lax.optimization_barrier(mixture)
    return (stream.astype(f32) + norm_rows(mixture, norm_gain[2])).astype(b16)


def solution(mesh):
    return jax.shard_map(
        on_device,
        mesh=mesh,
        in_specs=(
            P("sp", "tp"),
            P("sp", "tp"),
            P(None, "tp"),
            P("tp"),
            P(None, "tp"),
            P(None, "tp", None, None),
            P(None, "tp"),
            P(None, "tp", None, None),
            P(None, "tp"),
            P(("sp", "tp"), None),
            P(),
            P(),
            P("sp", None),
            P("sp", None),
            P("sp", None, "tp"),
            P("sp", None, "tp"),
            P("sp", "tp", None),
        ),
        out_specs=P(("sp", "tp"), None),
        check_vma=False,
    )
```

```python
import functools

import jax
import jax.numpy as jnp
from jax import lax
from jax.experimental import pallas as pl
from jax.experimental.pallas import tpu as pltpu
from jax.sharding import PartitionSpec as P

EPSILON = 1e-06
MESH = pl.DeviceIdType.MESH
HALO = 16
SUB = 8


def norm_rows(values, gain):
    floats = values.astype(jnp.float32)
    return floats * lax.rsqrt(jnp.mean(floats * floats, axis=-1, keepdims=True) + EPSILON) * gain


def slot_table(route_rows, experts, capacity):
    row_count, top_count = route_rows.shape
    flattened = route_rows.reshape(row_count * top_count)
    matches = flattened[:, None] == jnp.arange(experts, dtype=jnp.int32)[None, :]
    order = jnp.arange(row_count * top_count, dtype=jnp.int32)
    before = (order[None, :] < order[:, None]).astype(jnp.bfloat16)
    earlier_hits = jnp.dot(
        before, matches.astype(jnp.bfloat16), preferred_element_type=jnp.float32
    )
    position = jnp.sum(jnp.where(matches, earlier_hits, 0.0), axis=1).astype(jnp.int32)
    return (flattened * capacity + position).reshape(row_count, top_count)


def one_minus_exp(y):
    series = -y * (1.0 + y * (1.0 / 2) * (1.0 + y * (1.0 / 3) * (1.0 + y * 0.25 * (1.0 + y * 0.2))))
    return jnp.where(y > -0.1, series, 1.0 - jnp.exp(y))


def split_f32(x):
    high = x.astype(jnp.bfloat16)
    return high, (x - high.astype(jnp.float32)).astype(jnp.bfloat16)


def tile_scan(a, b, reverse):
    row = lax.broadcasted_iota(jnp.int32, a.shape, 1)
    step = 1
    while step < SUB:
        shift = SUB - step if reverse else step
        keep = row < SUB - step if reverse else row >= step
        a_prev = jnp.where(keep, pltpu.roll(a, shift, 1), 1.0)
        b_prev = jnp.where(keep, pltpu.roll(b, shift, 1), 0.0)
        b = b + a * b_prev
        a = a * a_prev
        step *= 2
    return a, b


def mixer_kernel(
    dims,
    mix_ref, gate_ref, cw_ref, cb_ref, soft_ref, rg_ref, rb_ref, ig_ref, ib_ref,
    res_ref, gain_ref, slots_ref, op_hbm, eg_hbm, eu_hbm, ed_hbm,
    stream_ref, arrived_hbm, gf_hbm, uf_hbm, df_hbm,
    xp, wh, wl, af, bf, ab, bb, mixed, tok, op, proj, normed, outgoing, halo, summ, ends,
    bg, bu, bd,
    op_sem, own_sem, halo_send, halo_recv, sum_send, sum_recv,
    mix_send, mix_recv, row_send, row_recv, dis_send, dis_recv, z_send, z_recv, c_send, c_recv,
):
    S, T, L, G, H = dims
    B = L // H
    seq, C = mix_ref.shape
    rows, D = res_ref.shape
    held = outgoing.shape[1] // S
    heads, hd = rg_ref.shape[1], rg_ref.shape[2]
    F = eg_hbm.shape[2]
    sp = lax.axis_index("sp")
    tp = lax.axis_index("tp")
    q = tp // G
    g = lax.rem(tp, G)
    half = q // B
    kind = lax.rem(q, B)

    def near_of(db, dg):
        return (half * B + lax.rem(kind + db, B)) * G + lax.rem(g + dg, G)

    def place_of(dq, dg):
        return lax.rem(q + dq, L) * G + lax.rem(g + dg, G)

    op_copy = pltpu.make_async_copy(op_hbm, op, op_sem)
    op_copy.start()
    own_in = [
        pltpu.make_async_copy(h.at[pl.ds(kind * H, H)], v, own_sem.at[i])
        for i, (h, v) in enumerate(((eg_hbm, bg), (eu_hbm, bu), (ed_hbm, bd)))
    ]
    for c in own_in:
        c.start()

    barrier = pltpu.get_barrier_semaphore()
    greeted = 0
    for ds in range(S):
        for dq in range(L):
            for dg in range(G):
                if (ds or dq or dg) and (ds == 0 or (dq == 0 and dg == 0)):
                    pl.semaphore_signal(
                        barrier, inc=1,
                        device_id=(lax.rem(sp + ds, S), place_of(dq, dg)),
                        device_id_type=MESH,
                    )
                    greeted += 1
    pl.semaphore_wait(barrier, greeted)

    def remote(src, dst, send, recv, sp_to, tp_to):
        return pltpu.make_async_remote_copy(
            src_ref=src, dst_ref=dst, send_sem=send, recv_sem=recv,
            device_id=(sp_to, tp_to), device_id_type=MESH,
        )

    to_next = remote(mix_ref.at[pl.ds(seq - HALO, HALO)], halo.at[0], halo_send.at[0],
                     halo_recv.at[0], lax.rem(sp + 1, S), tp)
    to_prev = remote(mix_ref.at[pl.ds(0, HALO)], halo.at[1], halo_send.at[1],
                     halo_recv.at[1], lax.rem(sp + S - 1, S), tp)
    to_next.start()
    to_prev.start()

    def full_slot(ref, axis, place):
        if len(ref.shape) == 4:
            return ref.at[:, place]
        start = pl.multiple_of(place * F, F)
        return ref.at[:, :, pl.ds(start, F)] if axis else ref.at[:, pl.ds(start, F), :]

    tensors = ((eg_hbm, gf_hbm, 1), (eu_hbm, uf_hbm, 1), (ed_hbm, df_hbm, 0))
    column = kind * G + g

    def z_copies(db):
        to_kind = lax.rem(kind + db, B)
        return [
            remote(src.at[pl.ds(to_kind * H, H)], full_slot(dst, axis, column), z_send.at[db, i],
                   z_recv.at[db, i], sp, near_of(db, 0))
            for i, (src, dst, axis) in enumerate(tensors)
        ]

    def core_copies(db, i, own):
        src, dst, axis = tensors[i]
        at = full_slot(dst, axis, lax.rem(kind + B - db, B) * G + g)
        return [
            remote(own if own is not None else at, at, c_send.at[db, dg, i], c_recv.at[db, dg, i],
                   sp, near_of(0, dg))
            for dg in range(1, G)
        ]

    z_all = {db: z_copies(db) for db in range(1, B)}
    for i in range(3):
        for db in range(1, B):
            z_all[db][i].start()
    own_out, core_all = [], {}
    for i, (src, dst, axis) in enumerate(tensors):
        core_all[0, i] = core_copies(0, i, src.at[pl.ds(kind * H, H)])
        for c in core_all[0, i]:
            c.start()
    for i, (buf, (src, dst, axis)) in enumerate(zip((bg, bu, bd), tensors)):
        own_in[i].wait()
        c = pltpu.make_async_copy(buf, full_slot(dst, axis, column), own_sem.at[3 + i])
        c.start()
        own_out.append(c)

    wh[...] = jnp.zeros_like(wh)
    wl[...] = jnp.zeros_like(wl)
    for k, ref in enumerate((rg_ref, ig_ref)):
        for sense in range(2):
            for h in range(heads):
                high, low = split_f32(ref[sense, h])
                col = (2 * sense + k) * C + h * hd
                wh[h * hd : (h + 1) * hd, col : col + hd] = high
                wl[h * hd : (h + 1) * hd, col : col + hd] = low
    xp[SUB : SUB + seq, :] = mix_ref[...].astype(jnp.float32)
    to_next.wait()
    to_prev.wait()
    tail = halo[0].astype(jnp.float32)[HALO - SUB : HALO]
    head = halo[1].astype(jnp.float32)[0:SUB]
    xp[0:SUB, :] = jnp.where(sp > 0, tail, 0.0)
    xp[SUB + seq : 2 * SUB + seq, :] = jnp.where(sp < S - 1, head, 0.0)

    R = min(128, seq)

    def gates(n, _):
        base = pl.multiple_of(n * R, R)
        window = xp[pl.ds(base, R + 2 * SUB), :]
        conv = cb_ref[...] + window[SUB - 2 : SUB - 2 + R] * cw_ref[0:1]
        for tap in range(1, cw_ref.shape[0]):
            conv = conv + window[SUB - 2 + tap : SUB - 2 + tap + R] * cw_ref[tap : tap + 1]
        high, low = split_f32(conv)
        for sense, (a_ref, b_ref) in enumerate(((af, bf), (ab, bb))):
            cols = slice(2 * sense * C, (2 * sense + 2) * C)
            pre = jnp.dot(high, wh[:, cols], preferred_element_type=jnp.float32)
            pre = pre + jnp.dot(low, wh[:, cols], preferred_element_type=jnp.float32)
            pre = pre + jnp.dot(high, wl[:, cols], preferred_element_type=jnp.float32)
            recur = jax.nn.sigmoid(pre[:, :C] + rb_ref[sense : sense + 1])
            inp = jax.nn.sigmoid(pre[:, C:] + ib_ref[sense : sense + 1])
            log_a = -8.0 * recur * soft_ref[sense : sense + 1]
            a = jnp.exp(log_a)
            b = jnp.sqrt(one_minus_exp(2.0 * log_a)) * (inp * conv)
            a, b = tile_scan(
                a.reshape(R // SUB, SUB, C), b.reshape(R // SUB, SUB, C), sense == 1
            )
            a_ref[pl.ds(base, R), :] = a.reshape(R, C)
            b_ref[pl.ds(base, R), :] = b.reshape(R, C)
        return 0

    lax.fori_loop(0, seq // R, gates, 0)

    tiles = seq // SUB

    def carry(t, held):
        sf, pf, sb, pb = held
        at = pl.ds(pl.multiple_of(t * SUB, SUB), SUB)
        a = af[at, :]
        s = bf[at, :] + a * sf
        p = a * pf
        af[at, :] = p
        bf[at, :] = s
        back = pl.ds(pl.multiple_of((tiles - 1 - t) * SUB, SUB), SUB)
        a = ab[back, :]
        s2 = bb[back, :] + a * sb
        p2 = a * pb
        ab[back, :] = p2
        bb[back, :] = s2
        return s[SUB - 1 : SUB], p[SUB - 1 : SUB], s2[0:1], p2[0:1]

    zero, one = jnp.zeros((1, C), jnp.float32), jnp.ones((1, C), jnp.float32)
    sf, pf, sb, pb = lax.fori_loop(0, tiles, carry, (zero, one, zero, one), unroll=4)
    summ[0:1, :] = sf
    summ[1:2, :] = pf
    summ[2:3, :] = sb
    summ[3:4, :] = pb
    sums = [
        remote(summ, ends.at[ds - 1], sum_send.at[ds - 1], sum_recv.at[ds - 1],
               lax.rem(sp + ds, S), tp)
        for ds in range(1, S)
    ]
    for c in sums:
        c.start()
    for c in sums:
        c.wait()
    fe, be = zero, zero
    for ds in range(S - 1, 0, -1):
        fe = jnp.where(sp >= ds, ends[ds - 1, 1:2, :] * fe + ends[ds - 1, 0:1, :], fe)
    for ds in range(1, S):
        be = jnp.where(sp + S - ds < S, ends[ds - 1, 3:4, :] * be + ends[ds - 1, 2:3, :], be)

    def join(n, _):
        at = pl.ds(pl.multiple_of(n * R, R), R)
        state = (bf[at, :] + af[at, :] * fe) + (bb[at, :] + ab[at, :] * be)
        mixed[at, :] = (state * jax.nn.gelu(gate_ref[at, :].astype(jnp.float32))).astype(
            jnp.bfloat16
        )
        return 0

    lax.fori_loop(0, seq // R, join, 0)

    def block_rows(place):
        return mixed.at[pl.ds(pl.multiple_of(place * rows, rows), rows), :]

    columns = pl.ds(pl.multiple_of(tp * C, C), C)
    moves = []
    for dq in range(L):
        for dg in range(G):
            if dq or dg:
                k = dq * G + dg
                to = place_of(dq, dg)
                moves.append(remote(block_rows(to), tok.at[:, columns], mix_send.at[k],
                                    mix_recv.at[k], sp, to))
    for c in moves:
        c.start()
    own_move = pltpu.make_async_copy(block_rows(tp), tok.at[:, columns], own_sem.at[6])
    own_move.start()
    op_copy.wait()
    own_move.wait()
    for c in moves:
        c.wait()

    def project(n, _):
        cols = pl.ds(pl.multiple_of(n * 256, 256), 256)
        proj[:, cols] = (
            jnp.dot(tok[...], op[:, cols], preferred_element_type=jnp.float32)
            .astype(jnp.bfloat16)
        )
        return 0

    lax.fori_loop(0, D // 256, project, 0)
    part = 32

    def norms(n, _):
        at = pl.ds(pl.multiple_of(n * part, part), part)
        s = (
            res_ref[at, :].astype(jnp.float32) + norm_rows(proj[at, :], gain_ref[0:1, :])
        ).astype(jnp.bfloat16)
        stream_ref[at, :] = s
        normed[q, at, :] = norm_rows(s, gain_ref[1:2, :]).astype(jnp.bfloat16)
        return 0

    lax.fori_loop(0, rows // part, norms, 0)
    shares = [
        remote(normed.at[q], normed.at[q], row_send.at[dq], row_recv.at[dq], sp, place_of(dq, 0))
        for dq in range(1, L)
    ]
    for c in shares:
        c.start()
    slot_id = lax.broadcasted_iota(jnp.int32, (S * held, rows), 0)
    sends = []
    for dq in range(L):
        origin = lax.rem(q + L - dq, L)
        if dq:
            shares[dq - 1].wait_recv()
        named = slots_ref[origin]
        hit = slot_id == named[0:1]
        for k in range(1, named.shape[0]):
            hit = hit | (slot_id == named[k : k + 1])
        selector = jnp.where(hit, 1.0, 0.0).astype(jnp.bfloat16)

        def dispatch(n, _):
            cols = pl.ds(pl.multiple_of(n * 256, 256), 256)
            outgoing[dq, :, cols] = (
                jnp.dot(selector, normed[origin, :, cols], preferred_element_type=jnp.float32)
                .astype(jnp.bfloat16)
            )
            return 0

        lax.fori_loop(0, D // 256, dispatch, 0)
        cap = held // H
        mine = sp * L + origin
        for ds in range(S):
            sp_to = lax.rem(sp + ds, S)
            for j in range(H):
                start = pl.multiple_of(sp_to * held + j * cap, cap)
                src, dst = outgoing.at[dq, pl.ds(start, cap), :], arrived_hbm.at[j, mine]
                if ds:
                    c = remote(src, dst, dis_send.at[dq, ds, j], dis_recv.at[dq, ds, j], sp_to, tp)
                else:
                    c = pltpu.make_async_copy(src, dst, dis_send.at[dq, ds, j])
                c.start()
                sends.append(c)
    for db in range(1, B):
        for i in range(3):
            z_all[db][i].wait_recv()
            core_all[db, i] = core_copies(db, i, None)
            for c in core_all[db, i]:
                c.start()
    for c in sends:
        c.wait()
    for c in shares:
        c.wait_send()
    for db in range(1, B):
        for c in z_all[db]:
            c.wait_send()
    for c in own_out:
        c.wait()
    for group in core_all.values():
        for c in group:
            c.wait()


def return_kernel(
    dims, rows_hbm, stream_ref, gain_ref, slots_ref, wt_ref, out_ref,
    back, part_out, part_in, total, ret_send, ret_recv, mix_send, mix_recv,
):
    S, T, L, G, H = dims
    sp = lax.axis_index("sp")
    tp = lax.axis_index("tp")
    q = tp // G
    g = lax.rem(tp, G)
    held = back.shape[1] // S
    cap = held // H
    rows, D = stream_ref.shape
    barrier = pltpu.get_barrier_semaphore()
    peers = [(lax.rem(sp + ds, S), tp) for ds in range(1, S)]
    peers += [(sp, lax.rem(q + dq, L) * G + g) for dq in range(1, L)]
    for peer in peers:
        pl.semaphore_signal(barrier, inc=1, device_id=peer, device_id_type=MESH)
    pl.semaphore_wait(barrier, len(peers))
    order = list(range(1, L)) + [0]
    copies = {dq: [] for dq in order}
    for dq in order:
        origin = lax.rem(q + dq, L)
        for ds in range(S):
            sp_to = lax.rem(sp + ds, S)
            for j in range(H):
                start = pl.multiple_of(sp * held + j * cap, cap)
                src, dst = rows_hbm.at[j, sp_to * L + origin], back.at[dq, pl.ds(start, cap), :]
                if ds:
                    c = pltpu.make_async_remote_copy(
                        src_ref=src, dst_ref=dst, send_sem=ret_send.at[dq, ds, j],
                        recv_sem=ret_recv.at[dq, ds, j], device_id=(sp_to, tp),
                        device_id_type=MESH,
                    )
                else:
                    c = pltpu.make_async_copy(src, dst, ret_send.at[dq, ds, j])
                c.start()
                copies[dq].append(c)
    slot_id = lax.broadcasted_iota(jnp.int32, (rows, S * held), 1)
    shares = []
    for dq in order:
        origin = lax.rem(q + dq, L)
        named, wts = slots_ref[origin], wt_ref[origin]
        table = jnp.zeros((rows, S * held), jnp.float32)
        for k in range(named.shape[1]):
            table = jnp.where(slot_id == named[:, k : k + 1], wts[:, k : k + 1], table)
        high, low = split_f32(table)
        for c in copies[dq]:
            c.wait()

        def combine(n, _):
            cols = pl.ds(pl.multiple_of(n * 256, 256), 256)
            values = back[dq, :, cols]
            mix = jnp.dot(high, values, preferred_element_type=jnp.float32)
            mix = mix + jnp.dot(low, values, preferred_element_type=jnp.float32)
            if dq:
                part_out[dq, :, cols] = mix.astype(jnp.bfloat16)
            else:
                total[:, cols] = mix
            return 0

        lax.fori_loop(0, D // 256, combine, 0)
        if dq:
            c = pltpu.make_async_remote_copy(
                src_ref=part_out.at[dq], dst_ref=part_in.at[dq], send_sem=mix_send.at[dq],
                recv_sem=mix_recv.at[dq], device_id=(sp, origin * G + g), device_id_type=MESH,
            )
            c.start()
            shares.append(c)
    for c in shares:
        c.wait()
    part = 32

    def finish(n, _):
        at = pl.ds(pl.multiple_of(n * part, part), part)
        mix = total[at, :]
        for dq in range(1, L):
            mix = mix + part_in[dq, at, :].astype(jnp.float32)
        mix = mix.astype(jnp.bfloat16)
        out_ref[at, :] = (
            stream_ref[at, :].astype(jnp.float32) + norm_rows(mix, gain_ref[2:3, :])
        ).astype(jnp.bfloat16)
        return 0

    lax.fori_loop(0, rows // part, finish, 0)


def on_device(
    mix_in, gate_in, conv_w, conv_b, decay_param, recur_gate, recur_bias, input_gate, input_bias,
    residual, out_proj, norm_gain, routes, route_wt, exp_gate, exp_up, exp_down,
):
    S, T = lax.axis_size("sp"), lax.axis_size("tp")
    L, D, F = exp_gate.shape
    G = T // L
    H = 2 if L % 2 == 0 and L > 2 else 1
    B = L // H
    dims = (S, T, L, G, H)
    seq, C = mix_in.shape
    rows = residual.shape[0]
    top_count = routes.shape[1]
    experts = L * S
    cap = 2 * rows * top_count // experts
    place = lax.axis_index("tp")
    lane, kind = place % G, (place // G) % B

    def same_lane(a):
        blocks = a.reshape(L, G, rows, top_count)
        return lax.dynamic_index_in_dim(blocks, lane, 1, False)

    slots = jax.vmap(lambda block: slot_table(block, experts, cap))(same_lane(routes))
    weights = same_lane(route_wt)
    within = slots % (L * cap) - kind * (H * cap)
    slots = jnp.where(
        (within >= 0) & (within < H * cap), slots // (L * cap) * (H * cap) + within, -1
    )
    soft = jax.nn.softplus(-decay_param)
    wide = F % 128 == 0
    vmem = pl.BlockSpec(memory_space=pltpu.VMEM)
    hbm = pl.BlockSpec(memory_space=pltpu.MemorySpace.HBM)
    b16, f32 = jnp.bfloat16, jnp.float32
    dma = pltpu.SemaphoreType.DMA
    sds = jax.ShapeDtypeStruct
    N = B * G
    up_shape = (H, D, N * F) if wide else (H, N, D, F)
    down_shape = (H, N * F, D) if wide else (H, N, F, D)
    stream, arrived, gate_full, up_full, down_full = pl.pallas_call(
        functools.partial(mixer_kernel, dims),
        out_shape=(
            sds((rows, D), b16), sds((H, S * L, cap, D), b16),
            sds(up_shape, b16), sds(up_shape, b16), sds(down_shape, b16),
        ),
        in_specs=[vmem] * 12 + [hbm] * 4,
        out_specs=(vmem, hbm, hbm, hbm, hbm),
        scratch_shapes=[
            pltpu.VMEM((seq + 2 * SUB, C), f32),
            pltpu.VMEM((C, 4 * C), b16),
            pltpu.VMEM((C, 4 * C), b16),
            pltpu.VMEM((seq, C), f32), pltpu.VMEM((seq, C), f32),
            pltpu.VMEM((seq, C), f32), pltpu.VMEM((seq, C), f32),
            pltpu.VMEM((seq, C), b16),
            pltpu.VMEM((rows, T * C), b16),
            pltpu.VMEM(out_proj.shape, b16),
            pltpu.VMEM((rows, D), b16),
            pltpu.VMEM((L, rows, D), b16),
            pltpu.VMEM((L, S * H * cap, D), b16),
            pltpu.VMEM((2, HALO, C), b16),
            pltpu.VMEM((SUB, C), f32),
            pltpu.VMEM((S - 1, SUB, C), f32),
            pltpu.VMEM((H, D, F), b16), pltpu.VMEM((H, D, F), b16), pltpu.VMEM((H, F, D), b16),
            dma, dma((8,)),
            dma((2,)), dma((2,)),
            dma((S - 1,)), dma((S - 1,)),
            dma((T,)), dma((T,)),
            dma((L,)), dma((L,)),
            dma((L, S, H)), dma((L, S, H)),
            dma((B, 3)), dma((B, 3)),
            dma((B, G, 3)), dma((B, G, 3)),
        ],
        compiler_params=pltpu.CompilerParams(
            collective_id=0, has_side_effects=True, vmem_limit_bytes=56 * 1024 * 1024
        ),
    )(
        mix_in, gate_in, conv_w, conv_b.reshape(1, C), soft, recur_gate, recur_bias, input_gate,
        input_bias, residual, norm_gain, slots.transpose(0, 2, 1), out_proj, exp_gate, exp_up, exp_down,
    )
    flat = arrived.reshape(H, S * L * cap, D)
    spec = "hmd,hdf->hmf" if wide else "hmd,hndf->hmnf"
    gate_act = jnp.einsum(spec, flat, gate_full, preferred_element_type=f32)
    up_act = jnp.einsum(spec, flat, up_full, preferred_element_type=f32)
    hidden = (jax.nn.silu(gate_act) * up_act).astype(b16).reshape(H, S * L * cap, N * F)
    out_rows = jnp.einsum(
        "hmf,hfd->hmd", hidden, down_full.reshape(H, N * F, D), preferred_element_type=f32
    ).astype(b16)
    return pl.pallas_call(
        functools.partial(return_kernel, dims),
        out_shape=sds((rows, D), b16),
        in_specs=[hbm] + [vmem] * 4,
        out_specs=vmem,
        scratch_shapes=[
            pltpu.VMEM((L, S * H * cap, D), b16),
            pltpu.VMEM((L, rows, D), b16),
            pltpu.VMEM((L, rows, D), b16),
            pltpu.VMEM((rows, D), f32),
            dma((L, S, H)), dma((L, S, H)),
            dma((L,)), dma((L,)),
        ],
        compiler_params=pltpu.CompilerParams(collective_id=1, has_side_effects=True),
    )(out_rows.reshape(H, S * L, cap, D), stream, norm_gain, slots, weights)


def solution(mesh):
    return jax.shard_map(
        on_device,
        mesh=mesh,
        in_specs=(
            P("sp", "tp"),
            P("sp", "tp"),
            P(None, "tp"),
            P("tp"),
            P(None, "tp"),
            P(None, "tp", None, None),
            P(None, "tp"),
            P(None, "tp", None, None),
            P(None, "tp"),
            P(("sp", "tp"), None),
            P(),
            P(),
            P("sp", None),
            P("sp", None),
            P("sp", None, "tp"),
            P("sp", None, "tp"),
            P("sp", "tp", None),
        ),
        out_specs=P(("sp", "tp"), None),
        check_vma=False,
    )
```

```python
import functools

import jax
import jax.numpy as jnp
from jax import lax
from jax.experimental import pallas as pl
from jax.experimental.pallas import tpu as pltpu
from jax.sharding import PartitionSpec as P

EPSILON = 1e-06
MESH = pl.DeviceIdType.MESH
HALO = 16
SUB = 8


def norm_rows(values, gain):
    floats = values.astype(jnp.float32)
    return floats * lax.rsqrt(jnp.mean(floats * floats, axis=-1, keepdims=True) + EPSILON) * gain


def slot_table(route_rows, experts, capacity):
    row_count, top_count = route_rows.shape
    flattened = route_rows.reshape(row_count * top_count)
    matches = flattened[:, None] == jnp.arange(experts, dtype=jnp.int32)[None, :]
    order = jnp.arange(row_count * top_count, dtype=jnp.int32)
    before = (order[None, :] < order[:, None]).astype(jnp.bfloat16)
    earlier_hits = jnp.dot(
        before, matches.astype(jnp.bfloat16), preferred_element_type=jnp.float32
    )
    position = jnp.sum(jnp.where(matches, earlier_hits, 0.0), axis=1).astype(jnp.int32)
    return (flattened * capacity + position).reshape(row_count, top_count)


def one_minus_exp(y):
    series = -y * (1.0 + y * (1.0 / 2) * (1.0 + y * (1.0 / 3) * (1.0 + y * 0.25 * (1.0 + y * 0.2))))
    return jnp.where(y > -0.1, series, 1.0 - jnp.exp(y))


def split_f32(x):
    high = x.astype(jnp.bfloat16)
    return high, (x - high.astype(jnp.float32)).astype(jnp.bfloat16)


def tile_scan(a, b, reverse):
    row = lax.broadcasted_iota(jnp.int32, a.shape, 1)
    step = 1
    while step < SUB:
        shift = SUB - step if reverse else step
        keep = row < SUB - step if reverse else row >= step
        a_prev = jnp.where(keep, pltpu.roll(a, shift, 1), 1.0)
        b_prev = jnp.where(keep, pltpu.roll(b, shift, 1), 0.0)
        b = b + a * b_prev
        a = a * a_prev
        step *= 2
    return a, b


def mixer_kernel(
    dims,
    mix_ref, gate_ref, cw_ref, cb_ref, soft_ref, rg_ref, rb_ref, ig_ref, ib_ref,
    res_ref, gain_ref, slots_ref, op_hbm, eg_hbm, eu_hbm, ed_hbm,
    stream_ref, arrived_hbm, gf_hbm, uf_hbm, df_hbm,
    xp, wh, wl, af, bf, ab, bb, mixed, tok, op, proj, normed, outgoing, halo, summ, ends,
    bg, bu, bd,
    op_sem, own_sem, halo_send, halo_recv, sum_send, sum_recv,
    mix_send, mix_recv, row_send, row_recv, dis_send, dis_recv, z_send, z_recv, c_send, c_recv,
):
    S, T, L, G, H = dims
    B = L // H
    seq, C = mix_ref.shape
    rows, D = res_ref.shape
    held = outgoing.shape[1] // S
    heads, hd = rg_ref.shape[1], rg_ref.shape[2]
    F = eg_hbm.shape[2]
    sp = lax.axis_index("sp")
    tp = lax.axis_index("tp")
    q = tp // G
    g = lax.rem(tp, G)
    half = q // B
    kind = lax.rem(q, B)

    def near_of(db, dg):
        return (half * B + lax.rem(kind + db, B)) * G + lax.rem(g + dg, G)

    def place_of(dq, dg):
        return lax.rem(q + dq, L) * G + lax.rem(g + dg, G)

    op_copy = pltpu.make_async_copy(op_hbm, op, op_sem)
    op_copy.start()
    own_in = [
        pltpu.make_async_copy(h.at[pl.ds(kind * H, H)], v, own_sem.at[i])
        for i, (h, v) in enumerate(((eg_hbm, bg), (eu_hbm, bu), (ed_hbm, bd)))
    ]
    for c in own_in:
        c.start()

    barrier = pltpu.get_barrier_semaphore()
    greeted = 0
    for ds in range(S):
        for dq in range(L):
            for dg in range(G):
                if (ds or dq or dg) and (ds == 0 or (dq == 0 and dg == 0)):
                    pl.semaphore_signal(
                        barrier, inc=1,
                        device_id=(lax.rem(sp + ds, S), place_of(dq, dg)),
                        device_id_type=MESH,
                    )
                    greeted += 1
    pl.semaphore_wait(barrier, greeted)

    def remote(src, dst, send, recv, sp_to, tp_to):
        return pltpu.make_async_remote_copy(
            src_ref=src, dst_ref=dst, send_sem=send, recv_sem=recv,
            device_id=(sp_to, tp_to), device_id_type=MESH,
        )

    to_next = remote(mix_ref.at[pl.ds(seq - HALO, HALO)], halo.at[0], halo_send.at[0],
                     halo_recv.at[0], lax.rem(sp + 1, S), tp)
    to_prev = remote(mix_ref.at[pl.ds(0, HALO)], halo.at[1], halo_send.at[1],
                     halo_recv.at[1], lax.rem(sp + S - 1, S), tp)
    to_next.start()
    to_prev.start()

    def full_slot(ref, axis, place):
        if len(ref.shape) == 4:
            return ref.at[:, place]
        start = pl.multiple_of(place * F, F)
        return ref.at[:, :, pl.ds(start, F)] if axis else ref.at[:, pl.ds(start, F), :]

    tensors = ((eg_hbm, gf_hbm, 1), (eu_hbm, uf_hbm, 1), (ed_hbm, df_hbm, 0))
    column = kind * G + g

    def z_copies(db):
        to_kind = lax.rem(kind + db, B)
        return [
            remote(src.at[pl.ds(to_kind * H, H)], full_slot(dst, axis, column), z_send.at[db, i],
                   z_recv.at[db, i], sp, near_of(db, 0))
            for i, (src, dst, axis) in enumerate(tensors)
        ]

    def core_copies(db, i, own):
        src, dst, axis = tensors[i]
        at = full_slot(dst, axis, lax.rem(kind + B - db, B) * G + g)
        return [
            remote(own if own is not None else at, at, c_send.at[db, dg, i], c_recv.at[db, dg, i],
                   sp, near_of(0, dg))
            for dg in range(1, G)
        ]

    z_all = {db: z_copies(db) for db in range(1, B)}
    for db in range(1, B):
        z_all[db][0].start()
    own_out, core_all = [], {}
    for i, (src, dst, axis) in enumerate(tensors):
        core_all[0, i] = core_copies(0, i, src.at[pl.ds(kind * H, H)])
        for c in core_all[0, i]:
            c.start()
    for i, (buf, (src, dst, axis)) in enumerate(zip((bg, bu, bd), tensors)):
        own_in[i].wait()
        c = pltpu.make_async_copy(buf, full_slot(dst, axis, column), own_sem.at[3 + i])
        c.start()
        own_out.append(c)

    wh[...] = jnp.zeros_like(wh)
    wl[...] = jnp.zeros_like(wl)
    for k, ref in enumerate((rg_ref, ig_ref)):
        for sense in range(2):
            for h in range(heads):
                high, low = split_f32(ref[sense, h])
                col = (2 * sense + k) * C + h * hd
                wh[h * hd : (h + 1) * hd, col : col + hd] = high
                wl[h * hd : (h + 1) * hd, col : col + hd] = low
    xp[SUB : SUB + seq, :] = mix_ref[...].astype(jnp.float32)
    to_next.wait()
    to_prev.wait()
    tail = halo[0].astype(jnp.float32)[HALO - SUB : HALO]
    head = halo[1].astype(jnp.float32)[0:SUB]
    xp[0:SUB, :] = jnp.where(sp > 0, tail, 0.0)
    xp[SUB + seq : 2 * SUB + seq, :] = jnp.where(sp < S - 1, head, 0.0)

    R = min(128, seq)

    def gates(n, _):
        base = pl.multiple_of(n * R, R)
        window = xp[pl.ds(base, R + 2 * SUB), :]
        conv = cb_ref[...] + window[SUB - 2 : SUB - 2 + R] * cw_ref[0:1]
        for tap in range(1, cw_ref.shape[0]):
            conv = conv + window[SUB - 2 + tap : SUB - 2 + tap + R] * cw_ref[tap : tap + 1]
        high, low = split_f32(conv)
        for sense, (a_ref, b_ref) in enumerate(((af, bf), (ab, bb))):
            cols = slice(2 * sense * C, (2 * sense + 2) * C)
            pre = jnp.dot(high, wh[:, cols], preferred_element_type=jnp.float32)
            pre = pre + jnp.dot(low, wh[:, cols], preferred_element_type=jnp.float32)
            pre = pre + jnp.dot(high, wl[:, cols], preferred_element_type=jnp.float32)
            recur = jax.nn.sigmoid(pre[:, :C] + rb_ref[sense : sense + 1])
            inp = jax.nn.sigmoid(pre[:, C:] + ib_ref[sense : sense + 1])
            log_a = -8.0 * recur * soft_ref[sense : sense + 1]
            a = jnp.exp(log_a)
            b = jnp.sqrt(one_minus_exp(2.0 * log_a)) * (inp * conv)
            a, b = tile_scan(
                a.reshape(R // SUB, SUB, C), b.reshape(R // SUB, SUB, C), sense == 1
            )
            a_ref[pl.ds(base, R), :] = a.reshape(R, C)
            b_ref[pl.ds(base, R), :] = b.reshape(R, C)
        return 0

    lax.fori_loop(0, seq // R, gates, 0)

    tiles = seq // SUB

    def carry(t, held):
        sf, pf, sb, pb = held
        at = pl.ds(pl.multiple_of(t * SUB, SUB), SUB)
        a = af[at, :]
        s = bf[at, :] + a * sf
        p = a * pf
        af[at, :] = p
        bf[at, :] = s
        back = pl.ds(pl.multiple_of((tiles - 1 - t) * SUB, SUB), SUB)
        a = ab[back, :]
        s2 = bb[back, :] + a * sb
        p2 = a * pb
        ab[back, :] = p2
        bb[back, :] = s2
        return s[SUB - 1 : SUB], p[SUB - 1 : SUB], s2[0:1], p2[0:1]

    zero, one = jnp.zeros((1, C), jnp.float32), jnp.ones((1, C), jnp.float32)
    sf, pf, sb, pb = lax.fori_loop(0, tiles, carry, (zero, one, zero, one), unroll=4)
    summ[0:1, :] = sf
    summ[1:2, :] = pf
    summ[2:3, :] = sb
    summ[3:4, :] = pb
    sums = [
        remote(summ, ends.at[ds - 1], sum_send.at[ds - 1], sum_recv.at[ds - 1],
               lax.rem(sp + ds, S), tp)
        for ds in range(1, S)
    ]
    for c in sums:
        c.start()
    for c in sums:
        c.wait()
    fe, be = zero, zero
    for ds in range(S - 1, 0, -1):
        fe = jnp.where(sp >= ds, ends[ds - 1, 1:2, :] * fe + ends[ds - 1, 0:1, :], fe)
    for ds in range(1, S):
        be = jnp.where(sp + S - ds < S, ends[ds - 1, 3:4, :] * be + ends[ds - 1, 2:3, :], be)

    def join(n, _):
        at = pl.ds(pl.multiple_of(n * R, R), R)
        state = (bf[at, :] + af[at, :] * fe) + (bb[at, :] + ab[at, :] * be)
        mixed[at, :] = (state * jax.nn.gelu(gate_ref[at, :].astype(jnp.float32))).astype(
            jnp.bfloat16
        )
        return 0

    lax.fori_loop(0, seq // R, join, 0)

    def block_rows(place):
        return mixed.at[pl.ds(pl.multiple_of(place * rows, rows), rows), :]

    columns = pl.ds(pl.multiple_of(tp * C, C), C)
    moves = []
    for dq in range(L):
        for dg in range(G):
            if dq or dg:
                k = dq * G + dg
                to = place_of(dq, dg)
                moves.append(remote(block_rows(to), tok.at[:, columns], mix_send.at[k],
                                    mix_recv.at[k], sp, to))
    for c in moves:
        c.start()
    own_move = pltpu.make_async_copy(block_rows(tp), tok.at[:, columns], own_sem.at[6])
    own_move.start()
    for db in range(1, B):
        z_all[db][1].start()
    op_copy.wait()
    own_move.wait()
    for c in moves:
        c.wait()

    def project(n, _):
        cols = pl.ds(pl.multiple_of(n * 256, 256), 256)
        proj[:, cols] = (
            jnp.dot(tok[...], op[:, cols], preferred_element_type=jnp.float32)
            .astype(jnp.bfloat16)
        )
        return 0

    lax.fori_loop(0, D // 256, project, 0)
    part = 32

    def norms(n, _):
        at = pl.ds(pl.multiple_of(n * part, part), part)
        s = (
            res_ref[at, :].astype(jnp.float32) + norm_rows(proj[at, :], gain_ref[0:1, :])
        ).astype(jnp.bfloat16)
        stream_ref[at, :] = s
        normed[q, at, :] = norm_rows(s, gain_ref[1:2, :]).astype(jnp.bfloat16)
        return 0

    lax.fori_loop(0, rows // part, norms, 0)
    shares = [
        remote(normed.at[q], normed.at[q], row_send.at[dq], row_recv.at[dq], sp, place_of(dq, 0))
        for dq in range(1, L)
    ]
    for c in shares:
        c.start()
    for db in range(1, B):
        z_all[db][2].start()
    slot_id = lax.broadcasted_iota(jnp.int32, (S * held, rows), 0)
    sends = []
    for dq in range(L):
        origin = lax.rem(q + L - dq, L)
        if dq:
            shares[dq - 1].wait_recv()
        named = slots_ref[origin]
        hit = slot_id == named[0:1]
        for k in range(1, named.shape[0]):
            hit = hit | (slot_id == named[k : k + 1])
        selector = jnp.where(hit, 1.0, 0.0).astype(jnp.bfloat16)

        def dispatch(n, _):
            cols = pl.ds(pl.multiple_of(n * 256, 256), 256)
            outgoing[dq, :, cols] = (
                jnp.dot(selector, normed[origin, :, cols], preferred_element_type=jnp.float32)
                .astype(jnp.bfloat16)
            )
            return 0

        lax.fori_loop(0, D // 256, dispatch, 0)
        cap = held // H
        mine = sp * L + origin
        for ds in range(S):
            sp_to = lax.rem(sp + ds, S)
            for j in range(H):
                start = pl.multiple_of(sp_to * held + j * cap, cap)
                src, dst = outgoing.at[dq, pl.ds(start, cap), :], arrived_hbm.at[j, mine]
                if ds:
                    c = remote(src, dst, dis_send.at[dq, ds, j], dis_recv.at[dq, ds, j], sp_to, tp)
                else:
                    c = pltpu.make_async_copy(src, dst, dis_send.at[dq, ds, j])
                c.start()
                sends.append(c)
    for db in range(1, B):
        for i in range(3):
            z_all[db][i].wait_recv()
            core_all[db, i] = core_copies(db, i, None)
            for c in core_all[db, i]:
                c.start()
    for c in sends:
        c.wait()
    for c in shares:
        c.wait_send()
    for db in range(1, B):
        for c in z_all[db]:
            c.wait_send()
    for c in own_out:
        c.wait()
    for group in core_all.values():
        for c in group:
            c.wait()


def return_kernel(
    dims, rows_hbm, stream_ref, gain_ref, slots_ref, wt_ref, out_ref,
    back, part_out, part_in, total, ret_send, ret_recv, mix_send, mix_recv,
):
    S, T, L, G, H = dims
    sp = lax.axis_index("sp")
    tp = lax.axis_index("tp")
    q = tp // G
    g = lax.rem(tp, G)
    held = back.shape[1] // S
    cap = held // H
    rows, D = stream_ref.shape
    barrier = pltpu.get_barrier_semaphore()
    peers = [(lax.rem(sp + ds, S), tp) for ds in range(1, S)]
    peers += [(sp, lax.rem(q + dq, L) * G + g) for dq in range(1, L)]
    for peer in peers:
        pl.semaphore_signal(barrier, inc=1, device_id=peer, device_id_type=MESH)
    pl.semaphore_wait(barrier, len(peers))
    order = list(range(1, L)) + [0]
    copies = {dq: [] for dq in order}
    for dq in order:
        origin = lax.rem(q + dq, L)
        for ds in range(S):
            sp_to = lax.rem(sp + ds, S)
            for j in range(H):
                start = pl.multiple_of(sp * held + j * cap, cap)
                src, dst = rows_hbm.at[j, sp_to * L + origin], back.at[dq, pl.ds(start, cap), :]
                if ds:
                    c = pltpu.make_async_remote_copy(
                        src_ref=src, dst_ref=dst, send_sem=ret_send.at[dq, ds, j],
                        recv_sem=ret_recv.at[dq, ds, j], device_id=(sp_to, tp),
                        device_id_type=MESH,
                    )
                else:
                    c = pltpu.make_async_copy(src, dst, ret_send.at[dq, ds, j])
                c.start()
                copies[dq].append(c)
    slot_id = lax.broadcasted_iota(jnp.int32, (rows, S * held), 1)
    shares = []
    for dq in order:
        origin = lax.rem(q + dq, L)
        named, wts = slots_ref[origin], wt_ref[origin]
        table = jnp.zeros((rows, S * held), jnp.float32)
        for k in range(named.shape[1]):
            table = jnp.where(slot_id == named[:, k : k + 1], wts[:, k : k + 1], table)
        high, low = split_f32(table)
        for c in copies[dq]:
            c.wait()

        def combine(n, _):
            cols = pl.ds(pl.multiple_of(n * 256, 256), 256)
            values = back[dq, :, cols]
            mix = jnp.dot(high, values, preferred_element_type=jnp.float32)
            mix = mix + jnp.dot(low, values, preferred_element_type=jnp.float32)
            if dq:
                part_out[dq, :, cols] = mix.astype(jnp.bfloat16)
            else:
                total[:, cols] = mix
            return 0

        lax.fori_loop(0, D // 256, combine, 0)
        if dq:
            c = pltpu.make_async_remote_copy(
                src_ref=part_out.at[dq], dst_ref=part_in.at[dq], send_sem=mix_send.at[dq],
                recv_sem=mix_recv.at[dq], device_id=(sp, origin * G + g), device_id_type=MESH,
            )
            c.start()
            shares.append(c)
    for c in shares:
        c.wait()
    part = 32

    def finish(n, _):
        at = pl.ds(pl.multiple_of(n * part, part), part)
        mix = total[at, :]
        for dq in range(1, L):
            mix = mix + part_in[dq, at, :].astype(jnp.float32)
        mix = mix.astype(jnp.bfloat16)
        out_ref[at, :] = (
            stream_ref[at, :].astype(jnp.float32) + norm_rows(mix, gain_ref[2:3, :])
        ).astype(jnp.bfloat16)
        return 0

    lax.fori_loop(0, rows // part, finish, 0)


def on_device(
    mix_in, gate_in, conv_w, conv_b, decay_param, recur_gate, recur_bias, input_gate, input_bias,
    residual, out_proj, norm_gain, routes, route_wt, exp_gate, exp_up, exp_down,
):
    S, T = lax.axis_size("sp"), lax.axis_size("tp")
    L, D, F = exp_gate.shape
    G = T // L
    H = 2 if L % 2 == 0 and L > 2 else 1
    B = L // H
    dims = (S, T, L, G, H)
    seq, C = mix_in.shape
    rows = residual.shape[0]
    top_count = routes.shape[1]
    experts = L * S
    cap = 2 * rows * top_count // experts
    place = lax.axis_index("tp")
    lane, kind = place % G, (place // G) % B

    def same_lane(a):
        blocks = a.reshape(L, G, rows, top_count)
        return lax.dynamic_index_in_dim(blocks, lane, 1, False)

    slots = jax.vmap(lambda block: slot_table(block, experts, cap))(same_lane(routes))
    weights = same_lane(route_wt)
    within = slots % (L * cap) - kind * (H * cap)
    slots = jnp.where(
        (within >= 0) & (within < H * cap), slots // (L * cap) * (H * cap) + within, -1
    )
    soft = jax.nn.softplus(-decay_param)
    wide = F % 128 == 0
    vmem = pl.BlockSpec(memory_space=pltpu.VMEM)
    hbm = pl.BlockSpec(memory_space=pltpu.MemorySpace.HBM)
    b16, f32 = jnp.bfloat16, jnp.float32
    dma = pltpu.SemaphoreType.DMA
    sds = jax.ShapeDtypeStruct
    N = B * G
    up_shape = (H, D, N * F) if wide else (H, N, D, F)
    down_shape = (H, N * F, D) if wide else (H, N, F, D)
    stream, arrived, gate_full, up_full, down_full = pl.pallas_call(
        functools.partial(mixer_kernel, dims),
        out_shape=(
            sds((rows, D), b16), sds((H, S * L, cap, D), b16),
            sds(up_shape, b16), sds(up_shape, b16), sds(down_shape, b16),
        ),
        in_specs=[vmem] * 12 + [hbm] * 4,
        out_specs=(vmem, hbm, hbm, hbm, hbm),
        scratch_shapes=[
            pltpu.VMEM((seq + 2 * SUB, C), f32),
            pltpu.VMEM((C, 4 * C), b16),
            pltpu.VMEM((C, 4 * C), b16),
            pltpu.VMEM((seq, C), f32), pltpu.VMEM((seq, C), f32),
            pltpu.VMEM((seq, C), f32), pltpu.VMEM((seq, C), f32),
            pltpu.VMEM((seq, C), b16),
            pltpu.VMEM((rows, T * C), b16),
            pltpu.VMEM(out_proj.shape, b16),
            pltpu.VMEM((rows, D), b16),
            pltpu.VMEM((L, rows, D), b16),
            pltpu.VMEM((L, S * H * cap, D), b16),
            pltpu.VMEM((2, HALO, C), b16),
            pltpu.VMEM((SUB, C), f32),
            pltpu.VMEM((S - 1, SUB, C), f32),
            pltpu.VMEM((H, D, F), b16), pltpu.VMEM((H, D, F), b16), pltpu.VMEM((H, F, D), b16),
            dma, dma((8,)),
            dma((2,)), dma((2,)),
            dma((S - 1,)), dma((S - 1,)),
            dma((T,)), dma((T,)),
            dma((L,)), dma((L,)),
            dma((L, S, H)), dma((L, S, H)),
            dma((B, 3)), dma((B, 3)),
            dma((B, G, 3)), dma((B, G, 3)),
        ],
        compiler_params=pltpu.CompilerParams(
            collective_id=0, has_side_effects=True, vmem_limit_bytes=56 * 1024 * 1024
        ),
    )(
        mix_in, gate_in, conv_w, conv_b.reshape(1, C), soft, recur_gate, recur_bias, input_gate,
        input_bias, residual, norm_gain, slots.transpose(0, 2, 1), out_proj, exp_gate, exp_up, exp_down,
    )
    flat = arrived.reshape(H, S * L * cap, D)
    spec = "hmd,hdf->hmf" if wide else "hmd,hndf->hmnf"
    gate_act = jnp.einsum(spec, flat, gate_full, preferred_element_type=f32)
    up_act = jnp.einsum(spec, flat, up_full, preferred_element_type=f32)
    hidden = (jax.nn.silu(gate_act) * up_act).astype(b16).reshape(H, S * L * cap, N * F)
    out_rows = jnp.einsum(
        "hmf,hfd->hmd", hidden, down_full.reshape(H, N * F, D), preferred_element_type=f32
    ).astype(b16)
    return pl.pallas_call(
        functools.partial(return_kernel, dims),
        out_shape=sds((rows, D), b16),
        in_specs=[hbm] + [vmem] * 4,
        out_specs=vmem,
        scratch_shapes=[
            pltpu.VMEM((L, S * H * cap, D), b16),
            pltpu.VMEM((L, rows, D), b16),
            pltpu.VMEM((L, rows, D), b16),
            pltpu.VMEM((rows, D), f32),
            dma((L, S, H)), dma((L, S, H)),
            dma((L,)), dma((L,)),
        ],
        compiler_params=pltpu.CompilerParams(collective_id=1, has_side_effects=True),
    )(out_rows.reshape(H, S * L, cap, D), stream, norm_gain, slots, weights)


def solution(mesh):
    return jax.shard_map(
        on_device,
        mesh=mesh,
        in_specs=(
            P("sp", "tp"),
            P("sp", "tp"),
            P(None, "tp"),
            P("tp"),
            P(None, "tp"),
            P(None, "tp", None, None),
            P(None, "tp"),
            P(None, "tp", None, None),
            P(None, "tp"),
            P(("sp", "tp"), None),
            P(),
            P(),
            P("sp", None),
            P("sp", None),
            P("sp", None, "tp"),
            P("sp", None, "tp"),
            P("sp", "tp", None),
        ),
        out_specs=P(("sp", "tp"), None),
        check_vma=False,
    )
```
